32 devices in a mesh: sp: 4 (over y, x), tp: 8 (over z, core).
Axes of the slice: x: 2, y: 2, z: 4, core: 2. Of those that a mesh axis runs over, the one named last changes fastest.
Arguments:
- resid: bfloat16 [2048, 2048], P(('sp', 'tp')), may hold values from -6 to 6
- query_a: bfloat16 [2048, 16, 128], P('sp', 'tp'), may hold values from -16 to 16
- key_a: bfloat16 [2048, 16, 128], P('sp', 'tp'), may hold values from -16 to 16
- value_a: bfloat16 [2048, 16, 128], P('sp', 'tp'), may hold values from -6 to 6
- query_b: bfloat16 [2048, 16, 64], P('sp', 'tp'), may hold values from -16 to 16
- key_b: bfloat16 [2048, 16, 64], P('sp', 'tp'), may hold values from -16 to 16
- value_b: bfloat16 [2048, 16, 64], P('sp', 'tp'), may hold values from -6 to 6
- mix_a: float32 [16], P('tp'), may hold values from 0.3 to 0.8
- mix_b: float32 [16], P('tp'), may hold values from 0.3 to 0.8
- head_gain_a: float32 [128], replicated, may hold values from 0.1 to 1.9
- head_gain_b: float32 [64], replicated, may hold values from 0.1 to 1.9
- proj_a: bfloat16 [2048, 2048], P('tp'), may hold values from -0.109375 to 0.109375
- proj_b: bfloat16 [1024, 2048], P('tp'), may hold values from -0.109375 to 0.109375
- norm_gain: float32 [2048], replicated, may hold values from 0.1 to 1.9
- route_ids: int32 [2048, 2], P(('sp', 'tp')), may hold values from 0 to 3, all different within a row; in each aligned block of 64 rows (0 to 63, 64 to 127, ...) at most 48 rows name the same one
- route_weights: float32 [2048, 2], P(('sp', 'tp')), may hold values from 0.2 to 1
- expert_gate: bfloat16 [4, 2048, 6144], P('sp', None, 'tp'), may hold values from -0.125 to 0.125
- expert_up: bfloat16 [4, 2048, 6144], P('sp', None, 'tp'), may hold values from -0.125 to 0.125
- expert_down: bfloat16 [4, 6144, 2048], P('sp', 'tp'), may hold values from -0.078125 to 0.078125
Outputs:
- out: bfloat16 [2048, 2048], P(('sp', 'tp'))
The draws below stay inside these ranges and needn't reach their ends.
Inputs may be any that keep to these rules, and one draw needn't show every extreme that they name: `route_ids`: each row names 2 different experts. Within the rows of one device (aligned blocks of 64 rows) no expert is named by more than 48 rows, and in every draw some device's block names some expert exactly 48 times.
All inputs are finite; a program needn't handle non-finite values.
Results may differ from the reference program's by a relative error of at most 0.02.
Values may be sent and summed in bfloat16 or wider, within the bound.
A program may use at most 128 MiB of HBM per device.

```python
import math
import jax
import jax.numpy as jnp
import numpy as np
from jax import lax

D = 2048
HEADS_A = 16
QK_A = 64
V_A = 128
HEADS_B = 16
QK_B = 32
V_B = 64
FF = 6144
TOP = 2
SEQ_DEV = 512
EXPERTS = 4
TOK_DEV = 64
CAP = 48
TOKENS = 2048
N_TP = 8


def drawn_pair(key, heads, width):
    shape = (TOKENS, heads, 2 * width)
    query = jnp.clip(jax.random.normal(jax.random.fold_in(key, 21), shape, jnp.float32) * 1.3, -8.0, 8.0)
    keys = jnp.clip(jax.random.normal(jax.random.fold_in(key, 22), shape, jnp.float32) * 1.3, -8.0, 8.0)
    return (query, keys)


def draw_query_a(key, part):
    return drawn_pair(jax.random.fold_in(key, 1), HEADS_A, QK_A)[0].astype(jnp.bfloat16)


def draw_key_a(key, part):
    return drawn_pair(jax.random.fold_in(key, 1), HEADS_A, QK_A)[1].astype(jnp.bfloat16)


def draw_query_b(key, part):
    return drawn_pair(jax.random.fold_in(key, 2), HEADS_B, QK_B)[0].astype(jnp.bfloat16)


def draw_key_b(key, part):
    return drawn_pair(jax.random.fold_in(key, 2), HEADS_B, QK_B)[1].astype(jnp.bfloat16)


def level_of(stream_key, shape, split, smallest, largest):
    def one(axis_at, parts):
        steps = jax.random.uniform(jax.random.fold_in(jax.random.fold_in(stream_key, 6), axis_at), (parts,), jnp.float32, smallest / len(split), largest / len(split))
        return jnp.repeat(jnp.exp(steps), shape[axis_at] // parts).reshape((-1,) + (1,) * (len(shape) - axis_at - 1))

    loudness = one(*split[0])
    for cut in split[1:]:
        loudness = loudness * one(*cut)
    return loudness


def routed_block(key, own, number, rows, number_of, top, most, skew):
    order = jax.random.permutation(key, number_of)
    packed, common = shares(number_of, rows * top, most, skew, True), shares(number_of, rows * top, most, skew, False)
    places = jnp.arange(number_of)

    def named(tallies, turn):
        used = int((tallies > 0).sum())
        fixed = max(1, used // 4)
        moved = fixed + (places - fixed + turn * (used - fixed)) % max(1, number_of - fixed)
        return jnp.zeros((number_of,), jnp.int32).at[order[jnp.where(places < fixed, places, moved)]].set(jnp.asarray(tallies, jnp.int32))

    tallies = jnp.where(number % 4 == 0, named(packed, number // 4), named(common, number - number // 4 - 1))
    mixed = jax.random.permutation(jax.random.fold_in(own, 3), number_of)
    source_of, sink = mixed[0:number_of // 2 * 2:2], mixed[1:number_of // 2 * 2:2]
    margin = jnp.minimum(tallies[source_of] - 1, most - tallies[sink]) // 2
    margin = jnp.where((source_of == order[0]) | (sink == order[0]) | (tallies[sink] == 0), 0, jnp.maximum(margin, 0))
    moved = jax.random.randint(jax.random.fold_in(own, 4), (number_of // 2,), 0, 1 << 20) % (margin + 1)
    tallies = tallies.at[source_of].add(-moved).at[sink].add(moved)
    items = jnp.searchsorted(jnp.cumsum(tallies), jnp.arange(rows * top), side="right").astype(jnp.int32)
    table = items.reshape(top, rows).T
    table = table[jax.random.permutation(jax.random.fold_in(own, 1), rows)]
    turn = jax.random.randint(jax.random.fold_in(own, 2), (rows, 1), 0, top)
    return jnp.take_along_axis(table, (jnp.arange(top)[None, :] + turn) % top, axis=1)


def shares(number_of, total, reach, skew, full):
    loads = [(1 << 20) // math.isqrt(grade ** skew) + 1 for grade in range(1, number_of + 1)]
    largest = reach if full else min(reach, max(-(-total // number_of), total * loads[0] // sum(loads)))
    least = 1 if total - largest >= number_of - 1 else 0
    given, spare = [largest] + [least] * (number_of - 1), total - largest - least * (number_of - 1)
    while spare > 0:
        movable = [i for i in range(1, number_of) if given[i] < largest] or [i for i in range(1, number_of) if given[i] < reach]
        mass, remaining = sum([loads[i] for i in movable]), spare
        for i in movable:
            more = min(reach - given[i], max(1, remaining * loads[i] // mass), spare)
            given[i] = given[i] + more
            spare = spare - more
    return np.array(given)


def gaussian(stream_key, dims, scale, most, shards=(), held_as=jnp.bfloat16):
    drawn = jax.random.normal(stream_key, dims, jnp.float32) * scale
    if len(shards) > 0:
        drawn = level_of(stream_key, dims, shards, -0.22, 0.18) * drawn
    return jnp.clip(drawn, min=-most, max=most).astype(held_as)


def setup_inputs(seed: int = 0) -> dict:
    streams_of = jax.random.split(jax.random.key(seed), 20)
    resid = gaussian(streams_of[0], (TOKENS, D), 1.0, 6.0, ((0, 32),))
    query_a = draw_query_a(jax.random.fold_in(streams_of[19], 71), 0)
    key_a = draw_key_a(jax.random.fold_in(streams_of[19], 71), 0)
    value_a = gaussian(streams_of[3], (TOKENS, HEADS_A, V_A), 1.0, 6.0, ((0, 4), (1, 8)))
    query_b = draw_query_b(jax.random.fold_in(streams_of[19], 71), 0)
    key_b = draw_key_b(jax.random.fold_in(streams_of[19], 71), 0)
    value_b = gaussian(streams_of[6], (TOKENS, HEADS_B, V_B), 1.0, 6.0, ((0, 4), (1, 8)))
    mix_a = jnp.clip(0.3 + 0.5 * jax.random.uniform(streams_of[7], (HEADS_A,), jnp.float32) ** level_of(streams_of[7], (HEADS_A,), ((0, 8),), -0.2, 0.2), 0.3, 0.8)
    mix_b = jnp.clip(0.3 + 0.5 * jax.random.uniform(streams_of[8], (HEADS_B,), jnp.float32) ** level_of(streams_of[8], (HEADS_B,), ((0, 8),), -0.2, 0.2), 0.3, 0.8)
    head_gain_a = jnp.clip(1.0 + 0.18 * jax.random.normal(streams_of[9], (V_A,), jnp.float32), 0.1, 1.9)
    head_gain_b = jnp.clip(1.0 + 0.18 * jax.random.normal(streams_of[10], (V_B,), jnp.float32), 0.1, 1.9)
    proj_a = gaussian(streams_of[11], (HEADS_A * V_A, D), (HEADS_A * V_A + HEADS_B * V_B) ** -0.5, 0.109375, ((0, 8),))
    proj_b = gaussian(streams_of[12], (HEADS_B * V_B, D), (HEADS_A * V_A + HEADS_B * V_B) ** -0.5, 0.109375, ((0, 8),))
    norm_gain = jnp.clip(1.0 + 0.18 * jax.random.normal(streams_of[13], (D,), jnp.float32), 0.1, 1.9)
    route_ids_keys = jax.random.split(jax.random.fold_in(streams_of[14], 1), TOKENS // TOK_DEV)
    route_ids_turns = jax.random.permutation(jax.random.fold_in(streams_of[14], 3), TOKENS // TOK_DEV)
    route_ids = jax.vmap(lambda own, number: routed_block(jax.random.fold_in(streams_of[14], 2), own, number, TOK_DEV, EXPERTS, TOP, CAP, 1))(route_ids_keys, route_ids_turns).reshape((TOKENS, TOP))
    route_weights = jnp.clip(0.2 + 0.8 * jax.random.uniform(streams_of[15], (TOKENS, TOP), jnp.float32) ** level_of(streams_of[15], (TOKENS, TOP), ((0, 32),), -0.2, 0.2), 0.2, 1.0)
    expert_gate = gaussian(streams_of[16], (EXPERTS, D, FF), D ** -0.5, 0.125, ((0, 4), (2, 8)))
    expert_up = gaussian(streams_of[17], (EXPERTS, D, FF), D ** -0.5, 0.125, ((0, 4), (2, 8)))
    expert_down = gaussian(streams_of[18], (EXPERTS, FF, D), FF ** -0.5, 0.078125, ((0, 4), (1, 8)))
    return {"resid": resid, "query_a": query_a, "key_a": key_a, "value_a": value_a, "query_b": query_b, "key_b": key_b, "value_b": value_b, "mix_a": mix_a, "mix_b": mix_b, "head_gain_a": head_gain_a, "head_gain_b": head_gain_b, "proj_a": proj_a, "proj_b": proj_b, "norm_gain": norm_gain, "route_ids": route_ids, "route_weights": route_weights, "expert_gate": expert_gate, "expert_up": expert_up, "expert_down": expert_down}


EPS = 1e-06
HEAD_SCALE = 1.0 - (0.8 - 0.6 * math.exp(-0.3))

def attend(query, key, value, mix, gain):
    length, heads, double = query.shape
    width = double // 2
    scale = 1.0 / math.sqrt(width)
    block_rows = SEQ_DEV // 2
    keys_float = key.astype(jnp.float32)
    values_float = value.astype(jnp.float32)
    key_pos = jnp.arange(length, dtype=jnp.int32)

    def one_block(index):
        first = index * block_rows
        block = lax.dynamic_slice_in_dim(query, first, block_rows, 0).astype(jnp.float32)
        query_pos = first + jnp.arange(block_rows, dtype=jnp.int32)
        allowed = key_pos[None, :] <= query_pos[:, None]
        results = []
        for which in range(2):
            scores = jnp.einsum('qhd,khd->hqk', block[:, :, which * width:(which + 1) * width], keys_float[:, :, which * width:(which + 1) * width]) * scale
            scores = jnp.where(allowed[None], scores, -jnp.inf)
            shifted = jnp.exp(scores - lax.optimization_barrier(jnp.max(scores, axis=2, keepdims=True)))
            sums = lax.optimization_barrier(jnp.sum(shifted, axis=2))
            rounded = lax.optimization_barrier(shifted.astype(jnp.bfloat16)).astype(jnp.float32)
            weighted = jnp.einsum('hqk,khv->qhv', rounded, values_float)
            results.append(weighted / jnp.transpose(sums)[:, :, None])
        return results[0] - mix[None, :, None] * results[1]
    mixed = lax.map(one_block, jnp.arange(length // block_rows, dtype=jnp.int32))
    mixed = mixed.reshape(length, heads, -1)
    normed = mixed * lax.rsqrt(lax.optimization_barrier(jnp.mean(mixed * mixed, axis=2, keepdims=True)) + EPS) * gain * HEAD_SCALE
    return normed.astype(jnp.bfloat16).reshape(length, -1)

def slot_numbers(route_rows, experts, capacity):
    count, top_count = route_rows.shape
    flat = route_rows.reshape(count * top_count)
    onehot = (flat[:, None] == jnp.arange(experts, dtype=jnp.int32)[None, :]).astype(jnp.int32)
    ranks = lax.optimization_barrier(jnp.sum((jnp.cumsum(onehot, axis=0) - onehot) * onehot, axis=1))
    return (flat * capacity + ranks).reshape(count, top_count)

def reference(resid, query_a, key_a, value_a, query_b, key_b, value_b, mix_a, mix_b, head_gain_a, head_gain_b, proj_a, proj_b, norm_gain, route_ids, route_weights, expert_gate, expert_up, expert_down):
    heads_a = attend(query_a, key_a, value_a, mix_a, head_gain_a)
    heads_b = attend(query_b, key_b, value_b, mix_b, head_gain_b)
    cols_a = heads_a.shape[1] // N_TP
    cols_b = heads_b.shape[1] // N_TP
    mixed = resid.astype(jnp.float32)
    for shard in range(N_TP):
        partial_sum = jnp.dot(heads_a[:, shard * cols_a:(shard + 1) * cols_a], proj_a[shard * cols_a:(shard + 1) * cols_a], preferred_element_type=jnp.float32)
        partial_sum = partial_sum + jnp.dot(heads_b[:, shard * cols_b:(shard + 1) * cols_b], proj_b[shard * cols_b:(shard + 1) * cols_b], preferred_element_type=jnp.float32)
        mixed = mixed + lax.optimization_barrier(partial_sum.astype(jnp.bfloat16)).astype(jnp.float32)
    normed = (mixed * lax.rsqrt(lax.optimization_barrier(jnp.mean(mixed * mixed, axis=1, keepdims=True)) + EPS) * norm_gain).astype(jnp.bfloat16)
    blocks = TOKENS // TOK_DEV
    local = jax.vmap(lambda rows_in: slot_numbers(rows_in, EXPERTS, CAP))(route_ids.reshape(blocks, TOK_DEV, TOP))
    row_index = (jnp.arange(blocks, dtype=jnp.int32)[:, None, None] * CAP + local % CAP).reshape(-1)
    expert_index = route_ids.reshape(-1)
    buffer = jnp.zeros((EXPERTS, blocks * CAP, D), jnp.bfloat16)
    buffer = buffer.at[expert_index, row_index].set(jnp.repeat(normed, TOP, axis=0))
    block_width = FF // N_TP

    def run_expert(operands):
        rows_in, gate_w, up_w, down_w = operands
        gate = jnp.dot(rows_in, gate_w, preferred_element_type=jnp.float32)
        upward = jnp.dot(rows_in, up_w, preferred_element_type=jnp.float32)
        hidden = (jax.nn.silu(gate) * upward).astype(jnp.bfloat16)
        summed = jnp.zeros((rows_in.shape[0], D), jnp.float32)
        for shard in range(N_TP):
            part = jnp.dot(hidden[:, shard * block_width:(shard + 1) * block_width], down_w[shard * block_width:(shard + 1) * block_width], preferred_element_type=jnp.float32)
            summed = summed + lax.optimization_barrier(part.astype(jnp.bfloat16)).astype(jnp.float32)
        return summed.astype(jnp.bfloat16)
    outputs = lax.map(run_expert, (buffer, expert_gate, expert_up, expert_down))
    picked = outputs[expert_index, row_index].reshape(TOKENS, TOP, D).astype(jnp.float32)
    result = mixed + lax.optimization_barrier(jnp.sum(route_weights[:, :, None] * picked, axis=1))
    return result.astype(jnp.bfloat16)
```

```python
import functools
import math

import jax
import jax.numpy as jnp
from jax import lax
from jax.experimental import pallas as pl
from jax.experimental.pallas import tpu as pltpu
from jax.sharding import PartitionSpec as P

EPS = 1e-06
NEG = -1e30
HEAD_SCALE = 1.0 - (0.8 - 0.6 * math.exp(-0.3))
KEY_STEP = 512


def partner(value, axis, apart):
    return lax.ppermute(value, axis, [(i, i ^ 1 << apart) for i in range(lax.axis_size(axis))])


def rms_scaled(values, gain):
    return values * lax.rsqrt(jnp.mean(values * values, axis=-1, keepdims=True) + EPS) * gain


def slot_numbers(route_rows, experts, capacity):
    count, top_count = route_rows.shape
    flat = route_rows.reshape(count * top_count)
    onehot = (flat[:, None] == jnp.arange(experts, dtype=jnp.int32)[None, :]).astype(jnp.int32)
    ranks = jnp.sum((jnp.cumsum(onehot, axis=0) - onehot) * onehot, axis=1)
    return (flat * capacity + ranks).reshape(count, top_count)


def empty_map(count, heads, width):
    return (
        jnp.zeros((count, heads, width), jnp.float32),
        jnp.full((heads, count), NEG, jnp.float32),
        jnp.zeros((heads, count), jnp.float32),
    )


def empty_group(query, value):
    return (
        empty_map(query.shape[0], query.shape[1], value.shape[2]),
        empty_map(query.shape[0], query.shape[1], value.shape[2]),
    )


def map_update(state, query, keys, values, allowed, scale):
    weighted, maximum, sums = state
    scores = jnp.einsum("qhd,khd->hqk", query, keys, preferred_element_type=jnp.float32) * scale
    scores = jnp.where(allowed[None], scores, NEG)
    fresh = jnp.maximum(maximum, jnp.max(scores, axis=2))
    weights = jnp.where(allowed[None], jnp.exp(scores - fresh[:, :, None]), 0.0)
    factor = jnp.exp(maximum - fresh)
    sums = sums * factor + jnp.sum(weights, axis=2)
    added = jnp.einsum(
        "hqk,khv->qhv", weights.astype(jnp.bfloat16), values, preferred_element_type=jnp.float32
    )
    weighted = weighted * jnp.transpose(factor)[:, :, None] + added
    return (weighted, fresh, sums)


def group_update(states, query, keys, values, allowed):
    width = query.shape[2] // 2
    scale = 1.0 / math.sqrt(width)
    return tuple(
        (
            map_update(
                states[which],
                query[:, :, which * width : (which + 1) * width],
                keys[:, :, which * width : (which + 1) * width],
                values,
                allowed,
                scale,
            )
            for which in range(2)
        )
    )


def set_update(carry, queries, pieces):
    rows_a, rows_b, query_pos = queries
    piece_key_a, piece_value_a, piece_key_b, piece_value_b = pieces
    length = piece_key_a.shape[0]
    step = math.gcd(length, KEY_STEP)
    latest = query_pos[-1]

    def inner(index, states):
        first = index * step

        def compute(current):
            keys_a = lax.dynamic_slice_in_dim(piece_key_a, first, step, 0)
            values_a = lax.dynamic_slice_in_dim(piece_value_a, first, step, 0)
            keys_b = lax.dynamic_slice_in_dim(piece_key_b, first, step, 0)
            values_b = lax.dynamic_slice_in_dim(piece_value_b, first, step, 0)
            key_pos = first + jnp.arange(step, dtype=jnp.int32)
            allowed = key_pos[None, :] <= query_pos[:, None]
            return (
                group_update(current[0], rows_a, keys_a, values_a, allowed),
                group_update(current[1], rows_b, keys_b, values_b, allowed),
            )

        return lax.cond(first <= latest, compute, lambda current: current, states)

    return lax.fori_loop(0, length // step, inner, carry)


def finish_group(states, mix, gain):
    outputs = [state[0] / jnp.transpose(state[2])[:, :, None] for state in states]
    mixed = outputs[0] - mix[None, :, None] * outputs[1]
    normed = rms_scaled(mixed, gain) * HEAD_SCALE
    return normed.astype(jnp.bfloat16).reshape(mixed.shape[0], -1)


def greet(axis, ways):
    me = lax.axis_index(axis)
    barrier = pltpu.get_barrier_semaphore()
    for apart in range(1, ways):
        pl.semaphore_signal(
            barrier,
            inc=1,
            device_id={axis: lax.rem(me + apart, ways)},
            device_id_type=pl.DeviceIdType.MESH,
        )
    pl.semaphore_wait(barrier, ways - 1)


def heads_kernel(
    ways, chunk, x_ref, par_ref, out_ref, got, heads, send_in, recv_in, send_out, recv_out
):
    me = lax.axis_index("sp")
    rows, wide = got.shape[1], out_ref.shape[2]
    greet("sp", ways)
    arriving = []
    for apart in range(1, ways):
        peer = lax.rem(me + apart, ways)
        copy = pltpu.make_async_remote_copy(
            src_ref=x_ref.at[peer],
            dst_ref=got.at[me],
            send_sem=send_in.at[apart],
            recv_sem=recv_in.at[apart],
            device_id={"sp": peer},
            device_id_type=pl.DeviceIdType.MESH,
        )
        copy.start()
        arriving.append(copy)
    got[me] = x_ref[me]
    for copy in arriving:
        copy.wait()
    gain, mix = par_ref[0:1, :], par_ref[1:2, :]
    scale, share = par_ref[2:3, 0:1], par_ref[3:4, 0:1]
    lane = lax.broadcasted_iota(jnp.int32, (chunk, wide), 1)

    def result_copy(block):
        return pltpu.make_async_remote_copy(
            src_ref=heads.at[block],
            dst_ref=out_ref.at[me],
            send_sem=send_out.at[block],
            recv_sem=recv_out.at[me],
            device_id={"sp": block},
            device_id_type=pl.DeviceIdType.MESH,
        )

    for block in reversed(range(ways)):
        length = (block + 1) * rows

        @pl.loop(0, rows // chunk)
        def _(step):
            first = pl.multiple_of(step * chunk, chunk)
            query = got[block, pl.ds(first, chunk), 0:wide]
            keys = got[0 : block + 1, :, wide : 2 * wide].reshape(length, wide)
            values = got[0 : block + 1, :, 2 * wide : 3 * wide].reshape(length, wide)
            row = first + block * rows + lax.broadcasted_iota(jnp.int32, (chunk, rows), 0)
            col = block * rows + lax.broadcasted_iota(jnp.int32, (chunk, rows), 1)
            parts = []
            for which in range(2):
                own = (lane < wide // 2) if which == 0 else (lane >= wide // 2)
                picked = jnp.where(own, query, jnp.zeros_like(query))
                scores = lax.dot_general(
                    picked, keys, (((1,), (1,)), ((), ())), preferred_element_type=jnp.float32
                )
                last = jnp.where(col <= row, scores[:, block * rows :], NEG)
                if block:
                    scores = jnp.concatenate([scores[:, : block * rows], last], axis=1)
                else:
                    scores = last
                top = jnp.max(scores, axis=1, keepdims=True)
                weights = jnp.exp2((scores - top) * scale)
                sums = jnp.sum(weights, axis=1, keepdims=True)
                mixed = jnp.dot(
                    weights.astype(jnp.bfloat16), values, preferred_element_type=jnp.float32
                )
                parts.append(mixed / sums)
            mixed = parts[0] - mix * parts[1]
            square = jnp.sum(mixed * mixed, axis=1, keepdims=True) * share
            heads[block, pl.ds(first, chunk), :] = (
                mixed * lax.rsqrt(square + EPS) * gain * HEAD_SCALE
            ).astype(jnp.bfloat16)

        @pl.when(me != block)
        def _():
            result_copy(block).start()

        @pl.when(me == block)
        def _():
            out_ref[block] = heads[block]

    for block in range(ways):

        @pl.when(me != block)
        def _():
            result_copy(block).wait_send()
            pltpu.make_async_remote_copy(
                src_ref=heads.at[block],
                dst_ref=out_ref.at[block],
                send_sem=send_out.at[block],
                recv_sem=recv_out.at[block],
                device_id={"sp": block},
                device_id_type=pl.DeviceIdType.MESH,
            ).wait_recv()


def wide_head(query, keys, values, wide, value_wide):
    rows, narrow = query.shape[0], query.shape[1] // 2

    def maps(array):
        halves = array.reshape(rows, 2, narrow)
        return jnp.pad(halves, ((0, 0), (0, 0), (0, wide - narrow))).reshape(rows, 2 * wide)

    padded = jnp.pad(values, ((0, 0), (0, value_wide - values.shape[1])))
    return jnp.concatenate([maps(query), maps(keys), padded], axis=1)


def whole_heads(query_a, key_a, value_a, query_b, key_b, value_b, mix_a, mix_b, gain_a, gain_b):
    ways = lax.axis_size("sp")
    heads_a, heads_b = query_a.shape[1], query_b.shape[1]
    rows, wide = query_a.shape[0], value_a.shape[2]
    half = query_a.shape[2] // 2
    order = [("a", h) for h in range(heads_a)]
    spot = heads_a // 2
    order = order[:spot] + [("b", h) for h in range(heads_b)] + order[spot:]
    units, params = [], []
    for group, head in order:
        if group == "a":
            query, keys, values, mix, gain = query_a, key_a, value_a, mix_a, gain_a
        else:
            query, keys, values, mix, gain = query_b, key_b, value_b, mix_b, gain_b
        units.append(wide_head(query[:, head], keys[:, head], values[:, head], half, wide))
        value_wide = values.shape[2]
        scale = math.log2(math.e) / math.sqrt(query.shape[2] // 2)
        params.append(
            jnp.stack(
                [
                    jnp.pad(gain, (0, wide - value_wide)),
                    jnp.full((wide,), mix[head]),
                    jnp.full((wide,), scale, jnp.float32),
                    jnp.full((wide,), 1.0 / value_wide, jnp.float32),
                ]
            )
        )
    par = lax.dynamic_index_in_dim(
        jnp.stack(params), lax.axis_index("sp"), axis=0, keepdims=False
    )
    chunk = math.gcd(rows, 128)
    got = pl.pallas_call(
        functools.partial(heads_kernel, ways, chunk),
        out_shape=jax.ShapeDtypeStruct((ways, rows, wide), jnp.bfloat16),
        in_specs=[pl.BlockSpec(memory_space=pltpu.VMEM)] * 2,
        out_specs=pl.BlockSpec(memory_space=pltpu.VMEM),
        scratch_shapes=[
            pltpu.VMEM((ways, rows, 3 * wide), jnp.bfloat16),
            pltpu.VMEM((ways, rows, wide), jnp.bfloat16),
            pltpu.SemaphoreType.DMA((ways,)),
            pltpu.SemaphoreType.DMA((ways,)),
            pltpu.SemaphoreType.DMA((ways,)),
            pltpu.SemaphoreType.DMA((ways,)),
        ],
        compiler_params=pltpu.CompilerParams(
            collective_id=1, has_side_effects=True, vmem_limit_bytes=48 << 20
        ),
    )(jnp.stack(units), jnp.pad(par, ((0, 4), (0, 0))))
    out_a = [got[at] for at, unit in enumerate(order) if unit[0] == "a"]
    out_b = [got[at, :, : value_b.shape[2]] for at, unit in enumerate(order) if unit[0] == "b"]
    return jnp.concatenate(out_a, axis=1), jnp.concatenate(out_b, axis=1)


def zigzag_heads(query_a, key_a, value_a, query_b, key_b, value_b, mix_a, mix_b, gain_a, gain_b):
    head_gain_a, head_gain_b = gain_a, gain_b
    seq_rows = query_a.shape[0]
    sp_ways = lax.axis_size("sp")
    place = lax.axis_index("sp")
    positions = place * seq_rows + jnp.arange(seq_rows, dtype=jnp.int32)
    levels = sp_ways.bit_length() - 1
    half = seq_rows // 2
    moved = jnp.concatenate(
        [query_a[half:].reshape(half, -1), query_b[half:].reshape(half, -1)], axis=1
    )
    for bit in range(levels):
        moved = partner(moved, "sp", bit)
    split_at = query_a.shape[1] * query_a.shape[2]
    far_a = moved[:, :split_at].reshape(half, query_a.shape[1], query_a.shape[2])
    far_b = moved[:, split_at:].reshape(half, query_b.shape[1], query_b.shape[2])
    far_pos = (sp_ways - 1 - place) * seq_rows + half + jnp.arange(half, dtype=jnp.int32)
    query_sets = ((query_a[:half], query_b[:half], positions[:half]), (far_a, far_b, far_pos))

    def fold_keys(carry, pieces):
        return tuple(
            (set_update(states, queries, pieces) for states, queries in zip(carry, query_sets))
        )

    initial = tuple(
        (
            (empty_group(queries[0], value_a), empty_group(queries[1], value_b))
            for queries in query_sets
        )
    )
    results = fold_keys(
        initial,
        (
            lax.all_gather(key_a, "sp", axis=0, tiled=True),
            lax.all_gather(value_a, "sp", axis=0, tiled=True),
            lax.all_gather(key_b, "sp", axis=0, tiled=True),
            lax.all_gather(value_b, "sp", axis=0, tiled=True),
        ),
    )
    finished = [
        (finish_group(states[0], mix_a, head_gain_a), finish_group(states[1], mix_b, head_gain_b))
        for states in results
    ]
    returned = jnp.concatenate([finished[1][0], finished[1][1]], axis=1)
    for bit in range(levels):
        returned = partner(returned, "sp", bit)
    width_a = finished[0][0].shape[1]
    heads_out_a = jnp.concatenate([finished[0][0], returned[:, :width_a]], axis=0)
    heads_out_b = jnp.concatenate([finished[0][1], returned[:, width_a:]], axis=0)
    return heads_out_a, heads_out_b


def per_device(
    resid,
    query_a,
    key_a,
    value_a,
    query_b,
    key_b,
    value_b,
    mix_a,
    mix_b,
    head_gain_a,
    head_gain_b,
    proj_a,
    proj_b,
    norm_gain,
    route_ids,
    route_weights,
    expert_gate,
    expert_up,
    expert_down,
):
    sp_ways = lax.axis_size("sp")
    fits = query_a.shape[1] + query_b.shape[1] == sp_ways
    fits = fits and query_a.shape[2] == value_a.shape[2] and value_b.shape[2] <= value_a.shape[2]
    attend = whole_heads if fits else zigzag_heads
    heads_out_a, heads_out_b = attend(
        query_a,
        key_a,
        value_a,
        query_b,
        key_b,
        value_b,
        mix_a,
        mix_b,
        head_gain_a,
        head_gain_b,
    )
    width = resid.shape[1]
    tok_rows = resid.shape[0]
    top_count = route_ids.shape[1]
    capacity = 3 * top_count * tok_rows // (2 * sp_ways)
    own_slots = slot_numbers(route_ids, sp_ways, capacity)
    term = jnp.dot(heads_out_a, proj_a, preferred_element_type=jnp.float32)
    term = term + jnp.dot(heads_out_b, proj_b, preferred_element_type=jnp.float32)
    mixed = resid.astype(jnp.float32) + lax.psum_scatter(
        lax.optimization_barrier(term.astype(jnp.bfloat16))
        .astype(jnp.float32)
        .astype(jnp.bfloat16),
        "tp",
        scatter_dimension=0,
        tiled=True,
    ).astype(jnp.float32)
    normed = rms_scaled(mixed, norm_gain).astype(jnp.bfloat16)
    lookup = jnp.arange(sp_ways * capacity, dtype=jnp.int32)[:, None]
    spread = jnp.zeros((sp_ways * capacity, tok_rows), jnp.float32)
    for which in range(top_count):
        spread = spread + (own_slots[:, which][None, :] == lookup).astype(jnp.float32)
    outgoing = jnp.dot(
        spread.astype(jnp.bfloat16), normed, preferred_element_type=jnp.float32
    ).astype(jnp.bfloat16)
    arrived = lax.all_to_all(
        outgoing.reshape(sp_ways, capacity, width), "sp", split_axis=0, concat_axis=0, tiled=True
    )
    piece = lax.all_gather(arrived.reshape(sp_ways * capacity, width), "tp", axis=0, tiled=True)
    gate = jnp.dot(piece, expert_gate[0], preferred_element_type=jnp.float32)
    upward = jnp.dot(piece, expert_up[0], preferred_element_type=jnp.float32)
    hidden = (jax.nn.silu(gate) * upward).astype(jnp.bfloat16)
    term = jnp.dot(hidden, expert_down[0], preferred_element_type=jnp.float32)
    summed = lax.psum_scatter(
        lax.optimization_barrier(term.astype(jnp.bfloat16))
        .astype(jnp.float32)
        .astype(jnp.bfloat16),
        "tp",
        scatter_dimension=0,
        tiled=True,
    )
    finished_rows = summed.reshape(sp_ways, capacity, width)
    back = lax.all_to_all(finished_rows, "sp", split_axis=0, concat_axis=0, tiled=True)
    picked = jnp.take(back.reshape(sp_ways * capacity, width), own_slots.reshape(-1), axis=0)
    picked = picked.reshape(tok_rows, top_count, width)
    output = mixed + jnp.sum(route_weights[:, :, None] * picked.astype(jnp.float32), axis=1)
    return output.astype(jnp.bfloat16)


def solution(mesh):
    placed = (
        P(("sp", "tp"), None),
        P("sp", "tp", None),
        P("sp", "tp", None),
        P("sp", "tp", None),
        P("sp", "tp", None),
        P("sp", "tp", None),
        P("sp", "tp", None),
        P("tp"),
        P("tp"),
        P(),
        P(),
        P("tp", None),
        P("tp", None),
        P(),
        P(("sp", "tp"), None),
        P(("sp", "tp"), None),
        P("sp", None, "tp"),
        P("sp", None, "tp"),
        P("sp", "tp", None),
    )
    return jax.shard_map(
        per_device, mesh=mesh, in_specs=placed, out_specs=P(("sp", "tp"), None), check_vma=False
    )
```

```python
import functools
import math

import jax
import jax.numpy as jnp
from jax import lax
from jax.experimental import pallas as pl
from jax.experimental.pallas import tpu as pltpu
from jax.sharding import PartitionSpec as P

EPS = 1e-06
NEG = -1e30
HEAD_SCALE = 1.0 - (0.8 - 0.6 * math.exp(-0.3))
KEY_STEP = 512


def partner(value, axis, apart):
    return lax.ppermute(value, axis, [(i, i ^ 1 << apart) for i in range(lax.axis_size(axis))])


def rms_scaled(values, gain):
    return values * lax.rsqrt(jnp.mean(values * values, axis=-1, keepdims=True) + EPS) * gain


def slot_numbers(route_rows, experts, capacity):
    count, top_count = route_rows.shape
    flat = route_rows.reshape(count * top_count)
    onehot = (flat[:, None] == jnp.arange(experts, dtype=jnp.int32)[None, :]).astype(jnp.int32)
    ranks = jnp.sum((jnp.cumsum(onehot, axis=0) - onehot) * onehot, axis=1)
    return (flat * capacity + ranks).reshape(count, top_count)


def empty_map(count, heads, width):
    return (
        jnp.zeros((count, heads, width), jnp.float32),
        jnp.full((heads, count), NEG, jnp.float32),
        jnp.zeros((heads, count), jnp.float32),
    )


def empty_group(query, value):
    return (
        empty_map(query.shape[0], query.shape[1], value.shape[2]),
        empty_map(query.shape[0], query.shape[1], value.shape[2]),
    )


def map_update(state, query, keys, values, allowed, scale):
    weighted, maximum, sums = state
    scores = jnp.einsum("qhd,khd->hqk", query, keys, preferred_element_type=jnp.float32) * scale
    scores = jnp.where(allowed[None], scores, NEG)
    fresh = jnp.maximum(maximum, jnp.max(scores, axis=2))
    weights = jnp.where(allowed[None], jnp.exp(scores - fresh[:, :, None]), 0.0)
    factor = jnp.exp(maximum - fresh)
    sums = sums * factor + jnp.sum(weights, axis=2)
    added = jnp.einsum(
        "hqk,khv->qhv", weights.astype(jnp.bfloat16), values, preferred_element_type=jnp.float32
    )
    weighted = weighted * jnp.transpose(factor)[:, :, None] + added
    return (weighted, fresh, sums)


def group_update(states, query, keys, values, allowed):
    width = query.shape[2] // 2
    scale = 1.0 / math.sqrt(width)
    return tuple(
        (
            map_update(
                states[which],
                query[:, :, which * width : (which + 1) * width],
                keys[:, :, which * width : (which + 1) * width],
                values,
                allowed,
                scale,
            )
            for which in range(2)
        )
    )


def set_update(carry, queries, pieces):
    rows_a, rows_b, query_pos = queries
    piece_key_a, piece_value_a, piece_key_b, piece_value_b = pieces
    length = piece_key_a.shape[0]
    step = math.gcd(length, KEY_STEP)
    latest = query_pos[-1]

    def inner(index, states):
        first = index * step

        def compute(current):
            keys_a = lax.dynamic_slice_in_dim(piece_key_a, first, step, 0)
            values_a = lax.dynamic_slice_in_dim(piece_value_a, first, step, 0)
            keys_b = lax.dynamic_slice_in_dim(piece_key_b, first, step, 0)
            values_b = lax.dynamic_slice_in_dim(piece_value_b, first, step, 0)
            key_pos = first + jnp.arange(step, dtype=jnp.int32)
            allowed = key_pos[None, :] <= query_pos[:, None]
            return (
                group_update(current[0], rows_a, keys_a, values_a, allowed),
                group_update(current[1], rows_b, keys_b, values_b, allowed),
            )

        return lax.cond(first <= latest, compute, lambda current: current, states)

    return lax.fori_loop(0, length // step, inner, carry)


def finish_group(states, mix, gain):
    outputs = [state[0] / jnp.transpose(state[2])[:, :, None] for state in states]
    mixed = outputs[0] - mix[None, :, None] * outputs[1]
    normed = rms_scaled(mixed, gain) * HEAD_SCALE
    return normed.astype(jnp.bfloat16).reshape(mixed.shape[0], -1)


def greet(axis, ways):
    me = lax.axis_index(axis)
    barrier = pltpu.get_barrier_semaphore()
    for apart in range(1, ways):
        pl.semaphore_signal(
            barrier,
            inc=1,
            device_id={axis: lax.rem(me + apart, ways)},
            device_id_type=pl.DeviceIdType.MESH,
        )
    pl.semaphore_wait(barrier, ways - 1)


def heads_kernel(
    ways, chunk, x_ref, par_ref, out_ref, got, heads, send_in, recv_in, send_out, recv_out
):
    me = lax.axis_index("sp")
    rows, wide = got.shape[1], out_ref.shape[2]
    greet("sp", ways)
    arriving = []
    for apart in range(1, ways):
        peer = lax.rem(me + apart, ways)
        copy = pltpu.make_async_remote_copy(
            src_ref=x_ref.at[peer],
            dst_ref=got.at[me],
            send_sem=send_in.at[apart],
            recv_sem=recv_in.at[apart],
            device_id={"sp": peer},
            device_id_type=pl.DeviceIdType.MESH,
        )
        copy.start()
        arriving.append(copy)
    got[me] = x_ref[me]
    for copy in arriving:
        copy.wait()
    gain, mix = par_ref[0:1, :], par_ref[1:2, :]
    scale, share = par_ref[2:3, 0:1], par_ref[3:4, 0:1]
    lane = lax.broadcasted_iota(jnp.int32, (chunk, wide), 1)

    def result_copy(block):
        return pltpu.make_async_remote_copy(
            src_ref=heads.at[block],
            dst_ref=out_ref.at[me],
            send_sem=send_out.at[block],
            recv_sem=recv_out.at[me],
            device_id={"sp": block},
            device_id_type=pl.DeviceIdType.MESH,
        )

    for block in reversed(range(ways)):
        length = (block + 1) * rows

        @pl.loop(0, rows // chunk)
        def _(step):
            first = pl.multiple_of(step * chunk, chunk)
            query = got[block, pl.ds(first, chunk), 0:wide]
            keys = got[0 : block + 1, :, wide : 2 * wide].reshape(length, wide)
            values = got[0 : block + 1, :, 2 * wide : 3 * wide].reshape(length, wide)
            row = first + block * rows + lax.broadcasted_iota(jnp.int32, (chunk, rows), 0)
            col = block * rows + lax.broadcasted_iota(jnp.int32, (chunk, rows), 1)
            parts = []
            for which in range(2):
                own = (lane < wide // 2) if which == 0 else (lane >= wide // 2)
                picked = jnp.where(own, query, jnp.zeros_like(query))
                scores = lax.dot_general(
                    picked, keys, (((1,), (1,)), ((), ())), preferred_element_type=jnp.float32
                )
                last = jnp.where(col <= row, scores[:, block * rows :], NEG)
                if block:
                    scores = jnp.concatenate([scores[:, : block * rows], last], axis=1)
                else:
                    scores = last
                top = jnp.max(scores, axis=1, keepdims=True)
                weights = jnp.exp2((scores - top) * scale)
                sums = jnp.sum(weights, axis=1, keepdims=True)
                mixed = jnp.dot(
                    weights.astype(jnp.bfloat16), values, preferred_element_type=jnp.float32
                )
                parts.append(mixed / sums)
            mixed = parts[0] - mix * parts[1]
            square = jnp.sum(mixed * mixed, axis=1, keepdims=True) * share
            heads[block, pl.ds(first, chunk), :] = (
                mixed * lax.rsqrt(square + EPS) * gain * HEAD_SCALE
            ).astype(jnp.bfloat16)

        @pl.when(me != block)
        def _():
            result_copy(block).start()

        @pl.when(me == block)
        def _():
            out_ref[block] = heads[block]

    for block in range(ways):

        @pl.when(me != block)
        def _():
            result_copy(block).wait_send()
            pltpu.make_async_remote_copy(
                src_ref=heads.at[block],
                dst_ref=out_ref.at[block],
                send_sem=send_out.at[block],
                recv_sem=recv_out.at[block],
                device_id={"sp": block},
                device_id_type=pl.DeviceIdType.MESH,
            ).wait_recv()


def wide_head(query, keys, values, wide, value_wide):
    rows, narrow = query.shape[0], query.shape[1] // 2

    def maps(array):
        halves = array.reshape(rows, 2, narrow)
        return jnp.pad(halves, ((0, 0), (0, 0), (0, wide - narrow))).reshape(rows, 2 * wide)

    padded = jnp.pad(values, ((0, 0), (0, value_wide - values.shape[1])))
    return jnp.concatenate([maps(query), maps(keys), padded], axis=1)


def whole_heads(query_a, key_a, value_a, query_b, key_b, value_b, mix_a, mix_b, gain_a, gain_b):
    ways = lax.axis_size("sp")
    heads_a, heads_b = query_a.shape[1], query_b.shape[1]
    rows, wide = query_a.shape[0], value_a.shape[2]
    half = query_a.shape[2] // 2
    order = [("a", h) for h in range(heads_a)]
    spot = heads_a // 2
    order = order[:spot] + [("b", h) for h in range(heads_b)] + order[spot:]
    units, params = [], []
    for group, head in order:
        if group == "a":
            query, keys, values, mix, gain = query_a, key_a, value_a, mix_a, gain_a
        else:
            query, keys, values, mix, gain = query_b, key_b, value_b, mix_b, gain_b
        units.append(wide_head(query[:, head], keys[:, head], values[:, head], half, wide))
        value_wide = values.shape[2]
        scale = math.log2(math.e) / math.sqrt(query.shape[2] // 2)
        params.append(
            jnp.stack(
                [
                    jnp.pad(gain, (0, wide - value_wide)),
                    jnp.full((wide,), mix[head]),
                    jnp.full((wide,), scale, jnp.float32),
                    jnp.full((wide,), 1.0 / value_wide, jnp.float32),
                ]
            )
        )
    par = lax.dynamic_index_in_dim(
        jnp.stack(params), lax.axis_index("sp"), axis=0, keepdims=False
    )
    chunk = math.gcd(rows, 128)
    got = pl.pallas_call(
        functools.partial(heads_kernel, ways, chunk),
        out_shape=jax.ShapeDtypeStruct((ways, rows, wide), jnp.bfloat16),
        in_specs=[pl.BlockSpec(memory_space=pltpu.VMEM)] * 2,
        out_specs=pl.BlockSpec(memory_space=pltpu.VMEM),
        scratch_shapes=[
            pltpu.VMEM((ways, rows, 3 * wide), jnp.bfloat16),
            pltpu.VMEM((ways, rows, wide), jnp.bfloat16),
            pltpu.SemaphoreType.DMA((ways,)),
            pltpu.SemaphoreType.DMA((ways,)),
            pltpu.SemaphoreType.DMA((ways,)),
            pltpu.SemaphoreType.DMA((ways,)),
        ],
        compiler_params=pltpu.CompilerParams(
            collective_id=1, has_side_effects=True, vmem_limit_bytes=48 << 20
        ),
    )(jnp.stack(units), jnp.pad(par, ((0, 4), (0, 0))))
    out_a = [got[at] for at, unit in enumerate(order) if unit[0] == "a"]
    out_b = [got[at, :, : value_b.shape[2]] for at, unit in enumerate(order) if unit[0] == "b"]
    return jnp.concatenate(out_a, axis=1), jnp.concatenate(out_b, axis=1)


def zigzag_heads(query_a, key_a, value_a, query_b, key_b, value_b, mix_a, mix_b, gain_a, gain_b):
    head_gain_a, head_gain_b = gain_a, gain_b
    seq_rows = query_a.shape[0]
    sp_ways = lax.axis_size("sp")
    place = lax.axis_index("sp")
    positions = place * seq_rows + jnp.arange(seq_rows, dtype=jnp.int32)
    levels = sp_ways.bit_length() - 1
    half = seq_rows // 2
    moved = jnp.concatenate(
        [query_a[half:].reshape(half, -1), query_b[half:].reshape(half, -1)], axis=1
    )
    for bit in range(levels):
        moved = partner(moved, "sp", bit)
    split_at = query_a.shape[1] * query_a.shape[2]
    far_a = moved[:, :split_at].reshape(half, query_a.shape[1], query_a.shape[2])
    far_b = moved[:, split_at:].reshape(half, query_b.shape[1], query_b.shape[2])
    far_pos = (sp_ways - 1 - place) * seq_rows + half + jnp.arange(half, dtype=jnp.int32)
    query_sets = ((query_a[:half], query_b[:half], positions[:half]), (far_a, far_b, far_pos))

    def fold_keys(carry, pieces):
        return tuple(
            (set_update(states, queries, pieces) for states, queries in zip(carry, query_sets))
        )

    initial = tuple(
        (
            (empty_group(queries[0], value_a), empty_group(queries[1], value_b))
            for queries in query_sets
        )
    )
    results = fold_keys(
        initial,
        (
            lax.all_gather(key_a, "sp", axis=0, tiled=True),
            lax.all_gather(value_a, "sp", axis=0, tiled=True),
            lax.all_gather(key_b, "sp", axis=0, tiled=True),
            lax.all_gather(value_b, "sp", axis=0, tiled=True),
        ),
    )
    finished = [
        (finish_group(states[0], mix_a, head_gain_a), finish_group(states[1], mix_b, head_gain_b))
        for states in results
    ]
    returned = jnp.concatenate([finished[1][0], finished[1][1]], axis=1)
    for bit in range(levels):
        returned = partner(returned, "sp", bit)
    width_a = finished[0][0].shape[1]
    heads_out_a = jnp.concatenate([finished[0][0], returned[:, :width_a]], axis=0)
    heads_out_b = jnp.concatenate([finished[0][1], returned[:, width_a:]], axis=0)
    return heads_out_a, heads_out_b


def remote(src, dst, send_sem, recv_sem, **where):
    return pltpu.make_async_remote_copy(
        src_ref=src,
        dst_ref=dst,
        send_sem=send_sem,
        recv_sem=recv_sem,
        device_id=where,
        device_id_type=pl.DeviceIdType.MESH,
    )


def greet_routes(places, chips):
    place, turn = lax.axis_index("sp"), lax.axis_index("tp")
    chip, core = lax.div(turn, 2), lax.rem(turn, 2)
    barrier = pltpu.get_barrier_semaphore()
    peers = [{"tp": 2 * chip + 1 - core}]
    peers += [{"tp": 2 * lax.rem(chip + apart, chips) + core} for apart in range(1, chips)]
    peers += [{"sp": lax.rem(place + apart, places)} for apart in range(1, places)]
    for peer in peers:
        pl.semaphore_signal(
            barrier, inc=1, device_id=peer, device_id_type=pl.DeviceIdType.MESH
        )
    pl.semaphore_wait(barrier, len(peers))


def dispatch_kernel(
    places, chips, cap, normed_ref, meta_ref, out_ref, near, stage, zs, zr, xs, xr, ps, pr
):
    place, turn = lax.axis_index("sp"), lax.axis_index("tp")
    chip, core = lax.div(turn, 2), lax.rem(turn, 2)
    other = 2 * chip + 1 - core
    rows = normed_ref.shape[0]
    greet_routes(places, chips)

    def near_copy(apart):
        peer = 2 * lax.rem(chip + apart, chips) + core
        return remote(normed_ref, near.at[apart], zs.at[apart], zr.at[apart], tp=peer)

    for apart in range(1, chips):
        near_copy(apart).start()

    def source(apart):
        return lax.rem(chip + chips - apart, chips)

    def route_copy(apart, away):
        expert = lax.rem(place + away, places)
        return remote(
            stage.at[apart, expert],
            out_ref.at[core, source(apart), place],
            xs.at[apart, away],
            xr.at[apart, away],
            sp=expert,
        )

    def pair_copy(apart, away):
        spot = out_ref.at[core, source(apart), lax.rem(place + places - away, places)]
        return remote(spot, spot, ps.at[apart, away], pr.at[apart, away], tp=other)

    slot = lax.broadcasted_iota(jnp.int32, (places * cap, rows), 0).astype(jnp.float32)
    for apart in range(chips):
        owner = 2 * source(apart) + core
        spread = jnp.zeros((places * cap, rows), jnp.float32)
        for which in range(2):
            own = meta_ref[owner, which : which + 1, 0:rows]
            spread = spread + jnp.where(slot == own, 1.0, 0.0)
        if apart:
            near_copy(apart).wait_recv()
            piece = near[apart]
        else:
            piece = normed_ref[...]
        sent = jnp.dot(spread.astype(jnp.bfloat16), piece, preferred_element_type=jnp.float32)
        stage[apart] = sent.astype(jnp.bfloat16).reshape(places, cap, sent.shape[1])
        for away in range(1, places):
            route_copy(apart, away).start()
        out_ref[core, source(apart), place] = stage[apart, place]
        pair_copy(apart, 0).start()
    for apart in range(chips):
        for away in range(1, places):
            route_copy(apart, away).wait_recv()
            pair_copy(apart, away).start()
    for apart in range(chips):
        if apart:
            near_copy(apart).wait_send()
        for away in range(places):
            if away:
                route_copy(apart, away).wait_send()
            pair_copy(apart, away).wait()


def combine_kernel(
    places,
    chips,
    cap,
    term_ref,
    meta_ref,
    mixed_ref,
    out_ref,
    pair,
    stage,
    back,
    leave,
    near,
    ps,
    pr,
    xs,
    xr,
    zs,
    zr,
):
    place, turn = lax.axis_index("sp"), lax.axis_index("tp")
    chip, core = lax.div(turn, 2), lax.rem(turn, 2)
    other = 2 * chip + 1 - core
    rows = mixed_ref.shape[0]
    greet_routes(places, chips)
    order = list(range(1, chips)) + [0]

    def source(apart):
        return lax.rem(chip + chips - apart, chips)

    def pair_copy(apart):
        return remote(
            term_ref.at[1 - core, source(apart)],
            pair.at[apart],
            ps.at[apart],
            pr.at[apart],
            tp=other,
        )

    def back_copy(apart, away):
        peer = lax.rem(place + away, places)
        return remote(
            stage.at[apart, peer],
            back.at[apart, place],
            xs.at[apart, away],
            xr.at[apart, away],
            sp=peer,
        )

    def near_copy(apart):
        peer = 2 * source(apart) + core
        return remote(leave.at[apart], near.at[apart], zs.at[apart], zr.at[apart], tp=peer)

    for apart in order:
        pair_copy(apart).start()
    for apart in order:
        pair_copy(apart).wait_recv()
        for expert in range(places):
            stage[apart, expert] = (
                term_ref[core, source(apart), expert].astype(jnp.float32)
                + pair[apart, expert].astype(jnp.float32)
            ).astype(jnp.bfloat16)
        for away in range(1, places):
            back_copy(apart, away).start()
        back[apart, place] = stage[apart, place]
    slot = lax.broadcasted_iota(jnp.int32, (places * cap, rows), 0).astype(jnp.float32)
    total = mixed_ref[...]
    for apart in order:
        owner = 2 * source(apart) + core
        gather = jnp.zeros((places * cap, rows), jnp.float32)
        for which in range(2):
            own = meta_ref[owner, which : which + 1, 0:rows]
            weight = meta_ref[owner, which + 2 : which + 3, 0:rows]
            gather = gather + jnp.where(slot == own, weight, 0.0)
        high = gather.astype(jnp.bfloat16)
        low = (gather - high.astype(jnp.float32)).astype(jnp.bfloat16)
        for away in range(1, places):
            back_copy(apart, away).wait_recv()
        held = back[apart].reshape(places * cap, back.shape[3])
        dims = (((0,), (0,)), ((), ()))
        part = lax.dot_general(high, held, dims, preferred_element_type=jnp.float32)
        part = part + lax.dot_general(low, held, dims, preferred_element_type=jnp.float32)
        if apart:
            leave[apart] = part.astype(jnp.bfloat16)
            near_copy(apart).start()
        else:
            total = total + part
    for apart in range(1, chips):
        near_copy(apart).wait_recv()
        total = total + near[apart].astype(jnp.float32)
    out_ref[...] = total.astype(jnp.bfloat16)
    for apart in range(chips):
        if apart:
            near_copy(apart).wait_send()
        pair_copy(apart).wait_send()
        for away in range(1, places):
            back_copy(apart, away).wait_send()


def vmem(count):
    return [pl.BlockSpec(memory_space=pltpu.VMEM)] * count


def routed_experts(mixed, normed, meta, capacity, expert_gate, expert_up, expert_down):
    places, chips = lax.axis_size("sp"), lax.axis_size("tp") // 2
    rows, width = normed.shape
    shape = (2, chips, places, capacity, width)
    sems = pltpu.SemaphoreType.DMA
    half = pltpu.VMEM((chips, places, capacity, width), jnp.bfloat16)
    piece_rows = pltpu.VMEM((chips, rows, width), jnp.bfloat16)
    piece = pl.pallas_call(
        functools.partial(dispatch_kernel, places, chips, capacity),
        out_shape=jax.ShapeDtypeStruct(shape, jnp.bfloat16),
        in_specs=vmem(2),
        out_specs=vmem(1)[0],
        scratch_shapes=[
            piece_rows,
            half,
            sems((chips,)),
            sems((chips,)),
            sems((chips, places)),
            sems((chips, places)),
            sems((chips, places)),
            sems((chips, places)),
        ],
        compiler_params=pltpu.CompilerParams(
            collective_id=2, has_side_effects=True, vmem_limit_bytes=48 << 20
        ),
    )(normed, meta).reshape(-1, width)
    gate = jnp.dot(piece, expert_gate[0], preferred_element_type=jnp.float32)
    upward = jnp.dot(piece, expert_up[0], preferred_element_type=jnp.float32)
    hidden = (jax.nn.silu(gate) * upward).astype(jnp.bfloat16)
    term = jnp.dot(hidden, expert_down[0], preferred_element_type=jnp.float32)
    return pl.pallas_call(
        functools.partial(combine_kernel, places, chips, capacity),
        out_shape=jax.ShapeDtypeStruct((rows, width), jnp.bfloat16),
        in_specs=vmem(3),
        out_specs=vmem(1)[0],
        scratch_shapes=[
            half,
            half,
            half,
            piece_rows,
            piece_rows,
            sems((chips,)),
            sems((chips,)),
            sems((chips, places)),
            sems((chips, places)),
            sems((chips,)),
            sems((chips,)),
        ],
        compiler_params=pltpu.CompilerParams(
            collective_id=3, has_side_effects=True, vmem_limit_bytes=56 << 20
        ),
    )(term.astype(jnp.bfloat16).reshape(shape), meta, mixed)


def per_device(
    resid,
    query_a,
    key_a,
    value_a,
    query_b,
    key_b,
    value_b,
    mix_a,
    mix_b,
    head_gain_a,
    head_gain_b,
    proj_a,
    proj_b,
    norm_gain,
    route_ids,
    route_weights,
    expert_gate,
    expert_up,
    expert_down,
):
    sp_ways = lax.axis_size("sp")
    fits = query_a.shape[1] + query_b.shape[1] == sp_ways
    fits = fits and query_a.shape[2] == value_a.shape[2] and value_b.shape[2] <= value_a.shape[2]
    attend = whole_heads if fits else zigzag_heads
    heads_out_a, heads_out_b = attend(
        query_a,
        key_a,
        value_a,
        query_b,
        key_b,
        value_b,
        mix_a,
        mix_b,
        head_gain_a,
        head_gain_b,
    )
    width = resid.shape[1]
    tok_rows = resid.shape[0]
    top_count = route_ids.shape[1]
    capacity = 3 * top_count * tok_rows // (2 * sp_ways)
    own_slots = slot_numbers(route_ids, sp_ways, capacity)
    term = jnp.dot(heads_out_a, proj_a, preferred_element_type=jnp.float32)
    term = term + jnp.dot(heads_out_b, proj_b, preferred_element_type=jnp.float32)
    mixed = resid.astype(jnp.float32) + lax.psum_scatter(
        lax.optimization_barrier(term.astype(jnp.bfloat16))
        .astype(jnp.float32)
        .astype(jnp.bfloat16),
        "tp",
        scatter_dimension=0,
        tiled=True,
    ).astype(jnp.float32)
    normed = rms_scaled(mixed, norm_gain).astype(jnp.bfloat16)
    tp_ways = lax.axis_size("tp")
    if top_count == 2 and capacity % 16 == 0 and tok_rows <= 128 and tp_ways % 2 == 0:
        meta = jnp.concatenate([own_slots.astype(jnp.float32).T, route_weights.T], axis=0)
        meta = jnp.pad(meta, ((0, 4), (0, 128 - tok_rows)))
        meta = lax.all_gather(meta, "tp", axis=0)
        return routed_experts(
            mixed, normed, meta, capacity, expert_gate, expert_up, expert_down
        )
    lookup = jnp.arange(sp_ways * capacity, dtype=jnp.int32)[:, None]
    spread = jnp.zeros((sp_ways * capacity, tok_rows), jnp.float32)
    for which in range(top_count):
        spread = spread + (own_slots[:, which][None, :] == lookup).astype(jnp.float32)
    outgoing = jnp.dot(
        spread.astype(jnp.bfloat16), normed, preferred_element_type=jnp.float32
    ).astype(jnp.bfloat16)
    arrived = lax.all_to_all(
        outgoing.reshape(sp_ways, capacity, width), "sp", split_axis=0, concat_axis=0, tiled=True
    )
    piece = lax.all_gather(arrived.reshape(sp_ways * capacity, width), "tp", axis=0, tiled=True)
    gate = jnp.dot(piece, expert_gate[0], preferred_element_type=jnp.float32)
    upward = jnp.dot(piece, expert_up[0], preferred_element_type=jnp.float32)
    hidden = (jax.nn.silu(gate) * upward).astype(jnp.bfloat16)
    term = jnp.dot(hidden, expert_down[0], preferred_element_type=jnp.float32)
    summed = lax.psum_scatter(
        lax.optimization_barrier(term.astype(jnp.bfloat16))
        .astype(jnp.float32)
        .astype(jnp.bfloat16),
        "tp",
        scatter_dimension=0,
        tiled=True,
    )
    finished_rows = summed.reshape(sp_ways, capacity, width)
    back = lax.all_to_all(finished_rows, "sp", split_axis=0, concat_axis=0, tiled=True)
    picked = jnp.take(back.reshape(sp_ways * capacity, width), own_slots.reshape(-1), axis=0)
    picked = picked.reshape(tok_rows, top_count, width)
    output = mixed + jnp.sum(route_weights[:, :, None] * picked.astype(jnp.float32), axis=1)
    return output.astype(jnp.bfloat16)


def solution(mesh):
    placed = (
        P(("sp", "tp"), None),
        P("sp", "tp", None),
        P("sp", "tp", None),
        P("sp", "tp", None),
        P("sp", "tp", None),
        P("sp", "tp", None),
        P("sp", "tp", None),
        P("tp"),
        P("tp"),
        P(),
        P(),
        P("tp", None),
        P("tp", None),
        P(),
        P(("sp", "tp"), None),
        P(("sp", "tp"), None),
        P("sp", None, "tp"),
        P("sp", None, "tp"),
        P("sp", "tp", None),
    )
    return jax.shard_map(
        per_device, mesh=mesh, in_specs=placed, out_specs=P(("sp", "tp"), None), check_vma=False
    )
```
